256 devices in a mesh: grp: 4 (over y, x), ep: 64 (over z, core).
Axes of the slice: x: 2, y: 2, z: 32, core: 2. Of those that a mesh axis runs over, the one named last changes fastest.
The devices are a block of a 4x8x32 slice.
Arguments:
- tokens: bfloat16 [32768, 2048], P(('grp', 'ep')), parts along dimension 0, may hold values from -6 to 6
- norm_gain: float32 [2048], replicated, may hold values from 0.1 to 1.9
- expert_ids: int32 [32768, 2], P(('grp', 'ep')), parts along dimension 0, may hold values from 0 to 15, all different within a row; in each aligned block of 128 rows (0 to 127, 128 to 255, ...) at most 32 rows name the same one
- route_weight: float32 [32768, 2], P(('grp', 'ep')), parts along dimension 0, may hold values from 0.1 to 1
- gate_weight: bfloat16 [64, 2048, 512], P('ep'), may hold values from -0.375 to 0.375
- up_weight: bfloat16 [64, 2048, 512], P('ep'), may hold values from -0.375 to 0.375
- down_weight: bfloat16 [64, 512, 2048], P('ep'), may hold values from -0.03125 to 0.03125
Outputs:
- combined: bfloat16 [32768, 2048], P(('grp', 'ep')), parts along dimension 0
The draws below stay inside these ranges and needn't reach their ends.
There are 4 independent parts, one for each index of `grp`. The reference program is written for one: setup_inputs(seed, part) draws one part's arguments, and reference() takes and returns one part's arrays. A program takes and returns all parts, laid end to end along the dimension named above; an argument that names none is the same for every part. Nothing has to cross between parts.
Inputs may be any that keep to these rules, and one draw needn't show every extreme that they name: `expert_ids`: each token names 2 different experts; among the tokens of one device no expert is named more than 32 times, and in every draw some expert is named exactly 32 times by the tokens of some device.
All inputs are finite; a program needn't handle non-finite values.
Results may differ from the reference program's by a relative error of at most 0.0078.
Values may be sent and summed in bfloat16 or wider, within the bound.
No kernel may reach another device: no remote copies, remote signals or barrier semaphores. Data moves between devices by JAX's collectives and lax.ppermute only.
A program may use at most 128 MiB of HBM per device.

```python
import math
import jax
import jax.numpy as jnp
import numpy as np
from jax import lax

D = 2048
FF = 2048
SPLIT = 4
FF_DEV = 512
TOP_K = 2
TOK_DEV = 128
EXPERTS = 16
CAP = 32
TOKENS = 8192
N_EP = 64


def levels(stream_key, extent, pieces, low, largest):
    factor_of, own = 1.0, jax.random.fold_in(stream_key, 6)
    for position, shards_of in pieces:
        steps = jnp.exp(jax.random.uniform(jax.random.fold_in(own, position), (shards_of,), jnp.float32, low / len(pieces), largest / len(pieces)))
        factor_of = factor_of * jnp.repeat(steps, extent[position] // shards_of).reshape([-1 if axis == position else 1 for axis in range(len(extent))])
    return factor_of


def assign_block(own_key, own, number, rows, amount, top, bound, skew):
    sequence = jax.random.permutation(own_key, amount)
    crowded, ordinary = shares(amount, rows * top, bound, skew, True), shares(amount, rows * top, bound, skew, False)
    places = jnp.arange(amount)

    def named(tallies, turn):
        used = int((tallies > 0).sum())
        fixed = max(1, used // 4)
        shifted = fixed + (places - fixed + turn * (used - fixed)) % max(1, amount - fixed)
        return jnp.zeros((amount,), jnp.int32).at[sequence[jnp.where(places < fixed, places, shifted)]].set(jnp.asarray(tallies, jnp.int32))

    tallies = jnp.where(number % 4 == 0, named(crowded, number // 4), named(ordinary, number - number // 4 - 1))
    mixed = jax.random.permutation(jax.random.fold_in(own, 3), amount)
    source_of, receiver = mixed[0:amount // 2 * 2:2], mixed[1:amount // 2 * 2:2]
    margin = jnp.minimum(tallies[source_of] - 1, bound - tallies[receiver]) // 2
    margin = jnp.where((source_of == sequence[0]) | (receiver == sequence[0]) | (tallies[receiver] == 0), 0, jnp.maximum(margin, 0))
    shifted = jax.random.randint(jax.random.fold_in(own, 4), (amount // 2,), 0, 1 << 20) % (margin + 1)
    tallies = tallies.at[source_of].add(-shifted).at[receiver].add(shifted)
    items = jnp.searchsorted(jnp.cumsum(tallies), jnp.arange(rows * top), side="right").astype(jnp.int32)
    table = items.reshape(top, rows).T
    table = table[jax.random.permutation(jax.random.fold_in(own, 1), rows)]
    turn = jax.random.randint(jax.random.fold_in(own, 2), (rows, 1), 0, top)
    return jnp.take_along_axis(table, (jnp.arange(top)[None, :] + turn) % top, axis=1)


def shares(amount, total, limit, slope, full):
    loads = [(1 << 20) // math.isqrt(rank ** slope) + 1 for rank in range(1, amount + 1)]
    largest = limit if full else min(limit, max(-(-total // amount), total * loads[0] // sum(loads)))
    least = 1 if total - largest >= amount - 1 else 0
    holding, rest = [largest] + [least] * (amount - 1), total - largest - least * (amount - 1)
    while rest > 0:
        candidates = [i for i in range(1, amount) if holding[i] < largest] or [i for i in range(1, amount) if holding[i] < limit]
        whole, budget = sum([loads[i] for i in candidates]), rest
        for i in candidates:
            extra = min(limit - holding[i], max(1, budget * loads[i] // whole), rest)
            holding[i] = holding[i] + extra
            rest = rest - extra
    return np.array(holding)


def normal_values(stream_key, dims, width, reach, cuts=(), held_as=jnp.bfloat16):
    drawn = width * jax.random.normal(stream_key, dims, jnp.float32)
    if cuts:
        drawn = drawn * levels(stream_key, dims, cuts, -0.22, 0.18)
    return jnp.clip(drawn, -reach, reach).astype(held_as)


def setup_inputs(seed: int = 0, part: int = 0) -> dict:
    key_list = jax.random.split(jax.random.key(seed), 8)
    part_keys = jax.random.split(jax.random.fold_in(key_list[7], part), 8)
    tokens = normal_values(part_keys[0], (TOKENS, D), 1.0, 6.0, ((0, 64),))
    norm_gain = jnp.clip(1.0 + 0.18 * jax.random.normal(key_list[1], (D,), jnp.float32), 0.1, 1.9)
    expert_ids_keys = jax.random.split(jax.random.fold_in(part_keys[2], 1), TOKENS // TOK_DEV)
    expert_ids_turns = jax.random.permutation(jax.random.fold_in(part_keys[2], 3), TOKENS // TOK_DEV)
    expert_ids = jax.vmap(lambda own, number: assign_block(jax.random.fold_in(part_keys[2], 2), own, number, TOK_DEV, EXPERTS, TOP_K, CAP, 2))(expert_ids_keys, expert_ids_turns).reshape((TOKENS, TOP_K))
    route_weight = jnp.clip(jnp.exp(math.log(1.0) - 2.3025851 * jax.random.uniform(part_keys[3], (TOKENS, TOP_K), jnp.float32) ** levels(part_keys[3], (TOKENS, TOP_K), ((0, 64),), -0.2, 0.2)), 0.1, 1.0)
    gate_weight = normal_values(key_list[4], (N_EP, D, FF_DEV), (D // 8) ** -0.5, 0.375, ((0, 64),))
    up_weight = normal_values(key_list[5], (N_EP, D, FF_DEV), (D // 8) ** -0.5, 0.375, ((0, 64),))
    down_weight = normal_values(key_list[6], (N_EP, FF_DEV, D), (16 * FF) ** -0.5, 0.03125, ((0, 64),))
    return dict(tokens=tokens, norm_gain=norm_gain, expert_ids=expert_ids, route_weight=route_weight, gate_weight=gate_weight, up_weight=up_weight, down_weight=down_weight)


EPSILON = 1e-05
clamp_limit = 7.0
sigmoid_slope = 1.702
row_block = 256

def reference(tokens, norm_gain, expert_ids, route_weight, gate_weight, up_weight, down_weight):
    values = tokens.astype(jnp.float32)
    center = values - lax.optimization_barrier(jnp.mean(values, axis=-1, keepdims=True))
    spread = lax.optimization_barrier(jnp.mean(center * center, axis=-1, keepdims=True))
    normed = (center * lax.rsqrt(spread + EPSILON) * norm_gain).astype(jnp.bfloat16)
    w_gate = gate_weight.reshape(EXPERTS, SPLIT, D, FF_DEV).transpose(0, 2, 1, 3).reshape(EXPERTS, D, FF)
    w_up = up_weight.reshape(EXPERTS, SPLIT, D, FF_DEV).transpose(0, 2, 1, 3).reshape(EXPERTS, D, FF)
    w_down = down_weight.reshape(EXPERTS, FF, D)
    assigned = TOKENS * TOP_K
    flat_ids = expert_ids.reshape(assigned).astype(jnp.int32)
    owners = jnp.arange(assigned, dtype=jnp.int32) // TOP_K
    ranking = jnp.argsort(flat_ids, stable=True).astype(jnp.int32)
    sorted_ids = flat_ids[ranking]
    counts = lax.optimization_barrier(jnp.sum((flat_ids[:, None] == jnp.arange(EXPERTS, dtype=jnp.int32)[None, :]).astype(jnp.int32), axis=0))
    starts = jnp.cumsum(counts) - counts
    padded_counts = (counts + row_block - 1) // row_block * row_block
    block_ends = jnp.cumsum(padded_counts)
    begins = block_ends - padded_counts
    target = (begins[sorted_ids] + jnp.arange(assigned, dtype=jnp.int32) - starts[sorted_ids]).astype(jnp.int32)
    blocks = -(-assigned // row_block) + EXPERTS
    slot_token = jnp.full((blocks * row_block,), TOKENS, jnp.int32).at[target].set(owners[ranking])
    first_rows = jnp.arange(blocks, dtype=jnp.int32) * row_block
    block_expert = jnp.minimum(lax.optimization_barrier(jnp.sum((first_rows[:, None] >= block_ends[None, :]).astype(jnp.int32), axis=1)), EXPERTS - 1).astype(jnp.int32)
    padded = jnp.concatenate([normed, jnp.zeros((1, D), jnp.bfloat16)], axis=0)
    gathered_rows = jnp.take(padded, slot_token, axis=0).reshape(blocks, row_block, D)

    def block_fn(operands):
        block_rows, expert = operands
        gate_pre = jnp.dot(block_rows, w_gate[expert], preferred_element_type=jnp.float32)
        up_pre = jnp.dot(block_rows, w_up[expert], preferred_element_type=jnp.float32)
        gate_cut = jnp.minimum(gate_pre, clamp_limit)
        up_cut = jnp.clip(up_pre, -clamp_limit, clamp_limit)
        active = ((up_cut + 1.0) * (gate_cut * jax.nn.sigmoid(gate_cut * sigmoid_slope))).astype(jnp.bfloat16)
        return jnp.dot(active, w_down[expert], preferred_element_type=jnp.float32).astype(jnp.bfloat16)
    outputs = lax.map(block_fn, (gathered_rows, block_expert)).reshape(blocks * row_block, D)
    sorted_out = jnp.take(outputs, target, axis=0)
    picked = jnp.zeros((assigned, D), jnp.bfloat16).at[ranking].set(sorted_out).reshape(TOKENS, TOP_K, D)
    combined = lax.optimization_barrier(jnp.sum(route_weight[:, :, None] * picked.astype(jnp.float32), axis=1))
    return combined.astype(jnp.bfloat16)
```

```python
from functools import partial

import jax
import jax.numpy as jnp
from jax import lax
from jax.experimental import pallas as pl
from jax.experimental.pallas import tpu as pltpu
from jax.sharding import PartitionSpec as P

INTERPRET = False
LANES = 128
SUB = 32
META = 16
EPSILON = 1e-05
clamp_limit = 7.0
sigmoid_slope = 1.702
f32 = jnp.float32
bf16 = jnp.bfloat16


def shifted(array, step):
    size = lax.axis_size("ep")
    return lax.ppermute(array, "ep", [(i, (i + step) % size) for i in range(size)])


def iota(shape, axis):
    return lax.broadcasted_iota(jnp.int32, shape, axis)


def reaches(ids, pair, parity, experts):
    half = experts // 2
    ahead = ids - pair
    ahead = jnp.where(ahead < 0, ahead + experts, ahead)
    behind = experts - ahead
    up_even = jnp.where(ahead < half, 2 * ahead + 1, 0)
    up_odd = jnp.where((ahead >= 1) & (ahead <= half), 2 * ahead, 0)
    down_even = jnp.where(ahead >= half, 2 * behind, 0)
    down_odd = jnp.where(ahead == 0, 1, jnp.where(ahead > half, 2 * behind + 1, 0))
    even = parity == 0
    return jnp.where(even, up_even, up_odd), jnp.where(even, down_even, down_odd)


def prepare_kernel(where_ref, tokens_ref, gain_ref, ids_ref, weight_ref,
                   upa_ref, upb_ref, downa_ref, downb_ref, upt_ref, downt_ref, *, experts):
    rows, width = tokens_ref.shape
    pair, parity = where_ref[0], where_ref[1]
    values = tokens_ref[...].astype(f32)
    center = values - jnp.mean(values, axis=-1, keepdims=True)
    spread = jnp.mean(center * center, axis=-1, keepdims=True)
    normed = (center * lax.rsqrt(spread + EPSILON) * gain_ref[...]).astype(bf16)

    ids = ids_ref[...].astype(f32)
    weights = weight_ref[...]
    high = weights.astype(bf16).astype(f32)
    middle = (weights - high).astype(bf16).astype(f32)
    low = weights - high - middle
    lane = iota((rows, LANES), 1)
    table = jnp.zeros((rows, LANES), f32)
    columns = [ids[:, 0:1], ids[:, 1:2]]
    for k in range(2):
        columns += [high[:, k:k + 1], middle[:, k:k + 1], low[:, k:k + 1]]
    for number, column in enumerate(columns):
        table = jnp.where(lane == number, column, table)
    meta = table.T
    meta_bf = meta[0:META, :].astype(bf16)
    first_c, second_c = ids_ref[:, 0:1], ids_ref[:, 1:2]
    first_r, second_r = meta[0:1, :].astype(jnp.int32), meta[1:2, :].astype(jnp.int32)
    reach_c = [jnp.maximum(a, b) for a, b in zip(
        reaches(first_c, pair, parity, experts), reaches(second_c, pair, parity, experts))]
    reach_r = [jnp.maximum(a, b) for a, b in zip(
        reaches(first_r, pair, parity, experts), reaches(second_r, pair, parity, experts))]
    sub_i, lane_i = iota((rows, rows), 0), iota((rows, rows), 1)
    for way, (a_ref, b_ref, t_ref) in enumerate(
            ((upa_ref, upb_ref, upt_ref), (downa_ref, downb_ref, downt_ref))):
        col, row = reach_c[way], reach_r[way]
        ahead_c = (row > col) | ((row == col) & (lane_i < sub_i))
        ahead_r = (col > row) | ((col == row) & (sub_i < lane_i))
        rank_c = jnp.sum(ahead_c.astype(f32), axis=1, keepdims=True).astype(jnp.int32)
        rank_r = jnp.sum(ahead_r.astype(f32), axis=0, keepdims=True).astype(jnp.int32)
        back = (rank_c == lane_i).astype(f32).astype(bf16)
        order = (rank_r == sub_i).astype(f32).astype(bf16)
        t_ref[...] = back
        ordered = jnp.dot(order, normed, preferred_element_type=f32).astype(bf16)
        a_ref[pl.ds(SUB * (width // LANES), META), :] = jnp.dot(
            meta_bf, back, preferred_element_type=f32).astype(bf16)
        for sub in range(4):
            put_sub(a_ref, b_ref, sub, ordered[SUB * sub:SUB * (sub + 1)], META)


def sub_place(sub, blocks, gap):
    return {0: (0, 0), 1: (1, 0), 2: (1, SUB * blocks), 3: (0, SUB * blocks + gap)}[sub]


def put_sub(a_ref, b_ref, sub, rows, gap):
    blocks = rows.shape[1] // LANES
    which, start = sub_place(sub, blocks, gap)
    ref = (a_ref, b_ref)[which]
    for c in range(blocks):
        ref[start + SUB * c:start + SUB * (c + 1), :] = rows[:, LANES * c:LANES * (c + 1)]


def get_block(refs, subs, blocks, gap, c, axis=0):
    parts = []
    for sub in range(subs):
        which, start = sub_place(sub, blocks, gap)
        parts.append(refs[which][start + SUB * c:start + SUB * (c + 1), :])
    return parts[0] if subs == 1 else jnp.concatenate(parts, axis=0)


def expert_kernel(*refs, specs, steps):
    count = len(specs)
    where_ref = refs[0]
    cursor = 1
    sources = []
    for subs, _ in specs:
        take = 2 if subs > 1 else 1
        sources.append(refs[cursor:cursor + take])
        cursor += take
    gates, ups, downs = refs[cursor:cursor + 2], refs[cursor + 2:cursor + 4], refs[cursor + 4:cursor + 6]
    cursor += 6
    results = []
    for subs, _ in specs:
        take = 2 if subs > 1 else 1
        results.append(refs[cursor:cursor + take])
        cursor += take
    rows_ref, sum_ref, hot_ref, factor_ref = refs[cursor:cursor + 4]
    width = rows_ref.shape[1]
    blocks = width // LANES
    step = pl.program_id(0)
    expert, parity = where_ref[0], where_ref[1]

    @pl.when(step == 0)
    def _():
        before = (iota((LANES, LANES), 0) < iota((LANES, LANES), 1)).astype(f32).astype(bf16)
        lane = iota((1, LANES), 1)
        for number, (subs, only) in enumerate(specs):
            meta = sources[number][0][SUB * blocks:SUB * blocks + META, :].astype(f32)
            target = expert.astype(f32)
            valid = lane < SUB * subs
            if only is not None:
                valid = valid & (lane < jnp.where(parity == only, LANES, 0))
            first = (meta[0:1] == target) & valid
            second = (meta[1:2] == target) & valid
            factor = jnp.where(first, (meta[2:3] + meta[3:4]) + meta[4:5], 0.0)
            factor = factor + jnp.where(second, (meta[5:6] + meta[6:7]) + meta[7:8], 0.0)
            match = jnp.where(first | second, 1.0, 0.0)
            slot = jnp.dot(jnp.broadcast_to(match, (16, LANES)).astype(bf16), before,
                           preferred_element_type=f32)[0:1]
            slot = jnp.where(match > 0.0, slot, -1.0)
            hot = (slot == iota((SUB, LANES), 0).astype(f32)).astype(f32)
            span = pl.ds(SUB * number, SUB)
            factor_ref[span, :] = jnp.broadcast_to(
                jnp.sum(hot * factor, axis=1, keepdims=True), (SUB, LANES))
            hot_ref[span, :] = hot
            hot = hot[:, :SUB * subs].astype(bf16)
            for c in range(blocks):
                rows_ref[span, LANES * c:LANES * (c + 1)] = jnp.dot(
                    hot, get_block(sources[number], subs, blocks, META, c),
                    preferred_element_type=f32).astype(bf16)

    def partial_sum(gate_ref, up_ref, down_ref):
        rows = rows_ref[...]
        gate = jnp.minimum(jnp.dot(rows, gate_ref[0], preferred_element_type=f32), clamp_limit)
        up = jnp.clip(jnp.dot(rows, up_ref[0], preferred_element_type=f32), -clamp_limit, clamp_limit)
        active = ((up + 1.0) * (gate * jax.nn.sigmoid(gate * sigmoid_slope))).astype(bf16)
        return jnp.dot(active, down_ref[0], preferred_element_type=f32)

    @pl.when(step == 0)
    def _():
        sum_ref[...] = partial_sum(gates[0], ups[0], downs[0])

    @pl.when((step > 0) & (step < steps))
    def _():
        sum_ref[...] += partial_sum(gates[0], ups[0], downs[0])

    @pl.when(step >= steps)
    def _():
        sum_ref[...] += partial_sum(gates[1], ups[1], downs[1])

    @pl.when(step == 2 * steps - 1)
    def _():
        for number, (subs, _) in enumerate(specs):
            span = pl.ds(SUB * number, SUB)
            weighted = (sum_ref[span, :] * factor_ref[span, 0:1]).astype(bf16)
            spread = hot_ref[span, :].T[:SUB * subs].astype(bf16)
            dense = jnp.dot(spread, weighted, preferred_element_type=f32).astype(bf16)
            pair = results[number]
            for sub in range(subs):
                put_sub(pair[0], pair[-1], sub, dense[SUB * sub:SUB * (sub + 1)], 0)


def finish_kernel(*refs):
    *messages, upt_ref, downt_ref, out_ref = refs
    width = out_ref.shape[1]
    blocks = width // LANES
    ways = ((upt_ref, messages[0:2]), (upt_ref, messages[2:4]), (downt_ref, messages[4:6]))
    for c in range(blocks):
        total = None
        for back_ref, pair in ways:
            part = jnp.dot(back_ref[...], get_block(pair, 4, blocks, 0, c), preferred_element_type=f32)
            total = part if total is None else total + part
        out_ref[:, LANES * c:LANES * (c + 1)] = total.astype(bf16)


VMEM = pl.BlockSpec(memory_space=pltpu.VMEM)
SMEM = pl.BlockSpec(memory_space=pltpu.SMEM)


def apply_experts(where, sources, specs, weights, partner_weights):
    width = weights[0].shape[1]
    hidden = weights[0].shape[2]
    tile = min(256, hidden)
    steps = hidden // tile
    blocks = width // LANES
    flat, out_shapes, in_specs, out_specs = [], [], [SMEM], []
    held = lambda shape: pl.BlockSpec(shape, lambda i: (0, 0), pipeline_mode=pl.Buffered(1))
    for (subs, _), pair in zip(specs, sources):
        flat += list(pair)
        in_specs += [held(x.shape) for x in pair]
        sizes = message_rows(subs, blocks)
        out_shapes += [jax.ShapeDtypeStruct((n, LANES), bf16) for n in sizes]
        out_specs += [held((n, LANES)) for n in sizes]
    own = lambda i: jnp.minimum(i, steps - 1)
    other = lambda i: jnp.maximum(i - steps, 0)
    for _ in range(2):
        in_specs += [pl.BlockSpec((1, width, tile), lambda i: (0, 0, own(i))),
                     pl.BlockSpec((1, width, tile), lambda i: (0, 0, other(i)))]
    in_specs += [pl.BlockSpec((1, tile, width), lambda i: (0, own(i), 0)),
                 pl.BlockSpec((1, tile, width), lambda i: (0, other(i), 0))]
    rows = SUB * len(specs)
    outs = pl.pallas_call(
        partial(expert_kernel, specs=tuple(specs), steps=steps),
        grid=(2 * steps,),
        in_specs=in_specs,
        out_specs=out_specs,
        out_shape=out_shapes,
        scratch_shapes=[pltpu.VMEM((rows, width), bf16), pltpu.VMEM((rows, width), f32),
                        pltpu.VMEM((rows, LANES), f32), pltpu.VMEM((rows, LANES), f32)],
        compiler_params=pltpu.CompilerParams(
            dimension_semantics=("arbitrary",), vmem_limit_bytes=56 * 1024 * 1024),
        cost_estimate=pl.CostEstimate(
            flops=6 * rows * width * 2 * hidden, transcendentals=0,
            bytes_accessed=12 * width * hidden),
        interpret=INTERPRET,
        name="experts",
    )(where, *flat, weights[0], partner_weights[0], weights[1], partner_weights[1],
      weights[2], partner_weights[2])
    results, cursor = [], 0
    for subs, _ in specs:
        take = len(message_rows(subs, blocks))
        results.append(list(outs[cursor:cursor + take]))
        cursor += take
    return results


def message_rows(subs, blocks):
    first = SUB * blocks * (2 if subs == 4 else 1)
    second = SUB * blocks * min(subs - 1, 2)
    return [first, second] if second else [first]


def body(tokens, norm_gain, expert_ids, route_weight, gate_weight, up_weight, down_weight):
    devices = lax.axis_size("ep")
    ring = devices // 2
    experts = ring // 2
    rows, width = tokens.shape
    blocks = width // LANES
    capacity = min(rows, 2 * rows * expert_ids.shape[1] // experts)
    hops = ring // 2
    chip = lax.axis_index("ep") // 2
    where = jnp.stack([chip // 2, chip % 2]).astype(jnp.int32)
    subs_at = [4] + [
        min(rows, capacity * (experts // 2 - (k + 1) // 2 + 1)) // SUB for k in range(1, hops + 1)]

    swap = [(i, i ^ 1) for i in range(devices)]
    weights = (gate_weight, up_weight, down_weight)
    partner = tuple(lax.ppermute(w, "ep", swap) for w in weights)

    full = message_rows(4, blocks)
    shapes = [jax.ShapeDtypeStruct((full[0] + META, LANES), bf16),
              jax.ShapeDtypeStruct((full[1], LANES), bf16)]
    upa, upb, downa, downb, up_back, down_back = pl.pallas_call(
        partial(prepare_kernel, experts=experts),
        in_specs=[SMEM, VMEM, VMEM, VMEM, VMEM],
        out_specs=[VMEM] * 6,
        out_shape=shapes * 2 + [jax.ShapeDtypeStruct((rows, rows), bf16)] * 2,
        interpret=INTERPRET,
        name="prepare",
    )(where, tokens, norm_gain.reshape(1, width), expert_ids, route_weight)

    def cut(pair, subs, gap):
        sizes = message_rows(subs, blocks)
        if gap:
            sizes[0] += META
        return [x[:n] if x.shape[0] != n else x for x, n in zip(pair, sizes)]

    arrived = {(0, 0): [upa, upb]}
    moving = {1: [upa, upb], -1: [downa, downb]}
    for k in range(1, hops + 1):
        for way in (1, -1):
            moving[way] = [shifted(x, 2 * way) for x in cut(moving[way], subs_at[k], True)]
            arrived[way, k] = moving[way]

    given = {}
    edges = [0, 4, 8, 12, 14, 16]
    edges = [e * hops // 16 for e in edges]
    for low, high in zip(edges[:-1], edges[1:]):
        keys = [(0, 0)] if low == 0 else []
        keys += [(way, k) for k in range(low + 1, high + 1) for way in (1, -1)]
        specs = [(subs_at[k], None if k < hops else (1 if way == 1 else 0)) for way, k in keys]
        for key, value in zip(keys, apply_experts(where, [arrived[k] for k in keys], specs,
                                                  weights, partner)):
            given[key] = value

    totals = {way: given[way, hops] for way in (1, -1)}
    for k in range(hops - 1, -1, -1):
        for way in (1, -1):
            came = [shifted(x, -2 * way) for x in totals[way]]
            if k == 0:
                totals[way] = came
                continue
            mine = given[way, k]
            joined = []
            for number, value in enumerate(mine):
                if number < len(came):
                    more = came[number]
                    padded = jnp.pad(more, ((0, value.shape[0] - more.shape[0]), (0, 0)))
                    value = (value.astype(f32) + padded.astype(f32)).astype(bf16)
                joined.append(value)
            totals[way] = joined

    return pl.pallas_call(
        finish_kernel,
        in_specs=[VMEM] * 8,
        out_specs=VMEM,
        out_shape=jax.ShapeDtypeStruct((rows, width), bf16),
        interpret=INTERPRET,
        name="finish",
    )(*given[0, 0], *totals[1], *totals[-1], up_back, down_back)


def solution(mesh):
    placed = (
        P(("grp", "ep"), None),
        P(),
        P(("grp", "ep"), None),
        P(("grp", "ep"), None),
        P("ep", None, None),
        P("ep", None, None),
        P("ep", None, None),
    )
    return jax.shard_map(
        body, mesh=mesh, in_specs=placed, out_specs=P(("grp", "ep"), None), check_vma=False
    )
```

```python
from functools import partial

import jax
import jax.numpy as jnp
from jax import lax
from jax.experimental import pallas as pl
from jax.experimental.pallas import tpu as pltpu
from jax.sharding import PartitionSpec as P


INTERPRET = False
LANES = 128
SUB = 32
STRIDE = 2
META = 16
EPSILON = 1e-05
clamp_limit = 7.0
sigmoid_slope = 1.702
f32 = jnp.float32
bf16 = jnp.bfloat16


def shifted(array, step):
    size = lax.axis_size("ep")
    return lax.ppermute(array, "ep", [(i, (i + step) % size) for i in range(size)])


def iota(shape, axis):
    return lax.broadcasted_iota(jnp.int32, shape, axis)


def reaches(ids, pair, parity, experts):
    half = experts // 2
    ahead = ids - pair
    ahead = jnp.where(ahead < 0, ahead + experts, ahead)
    behind = experts - ahead
    up_even = jnp.where(ahead < half, 2 * ahead + 1, 0)
    up_odd = jnp.where((ahead >= 1) & (ahead <= half), 2 * ahead, 0)
    down_even = jnp.where(ahead >= half, 2 * behind, 0)
    down_odd = jnp.where(ahead == 0, 1, jnp.where(ahead > half, 2 * behind + 1, 0))
    even = parity == 0
    return jnp.where(even, up_even, up_odd), jnp.where(even, down_even, down_odd)


def prepare_kernel(where_ref, tokens_ref, gain_ref, ids_ref, weight_ref,
                   upa_ref, upb_ref, downa_ref, downb_ref, upt_ref, downt_ref, *, experts):
    rows, width = tokens_ref.shape
    pair, parity = where_ref[0], where_ref[1]
    values = tokens_ref[...].astype(f32)
    center = values - jnp.mean(values, axis=-1, keepdims=True)
    spread = jnp.mean(center * center, axis=-1, keepdims=True)
    normed = (center * lax.rsqrt(spread + EPSILON) * gain_ref[...]).astype(bf16)

    ids = ids_ref[...].astype(f32)
    weights = weight_ref[...]
    high = weights.astype(bf16).astype(f32)
    middle = (weights - high).astype(bf16).astype(f32)
    low = weights - high - middle
    lane = iota((rows, LANES), 1)
    table = jnp.zeros((rows, LANES), f32)
    columns = [ids[:, 0:1], ids[:, 1:2]]
    for k in range(2):
        columns += [high[:, k:k + 1], middle[:, k:k + 1], low[:, k:k + 1]]
    for number, column in enumerate(columns):
        table = jnp.where(lane == number, column, table)
    meta = table.T
    meta_bf = meta[0:META, :].astype(bf16)
    first_c, second_c = ids_ref[:, 0:1], ids_ref[:, 1:2]
    first_r, second_r = meta[0:1, :].astype(jnp.int32), meta[1:2, :].astype(jnp.int32)
    reach_c = [jnp.maximum(a, b) for a, b in zip(
        reaches(first_c, pair, parity, experts), reaches(second_c, pair, parity, experts))]
    reach_r = [jnp.maximum(a, b) for a, b in zip(
        reaches(first_r, pair, parity, experts), reaches(second_r, pair, parity, experts))]
    sub_i, lane_i = iota((rows, rows), 0), iota((rows, rows), 1)
    for way, (a_ref, b_ref, t_ref) in enumerate(
            ((upa_ref, upb_ref, upt_ref), (downa_ref, downb_ref, downt_ref))):
        col, row = reach_c[way], reach_r[way]
        ahead_c = (row > col) | ((row == col) & (lane_i < sub_i))
        ahead_r = (col > row) | ((col == row) & (sub_i < lane_i))
        rank_c = jnp.sum(ahead_c.astype(f32), axis=1, keepdims=True).astype(jnp.int32)
        rank_r = jnp.sum(ahead_r.astype(f32), axis=0, keepdims=True).astype(jnp.int32)
        back = (rank_c == lane_i).astype(f32).astype(bf16)
        order = (rank_r == sub_i).astype(f32).astype(bf16)
        t_ref[...] = back
        ordered = jnp.dot(order, normed, preferred_element_type=f32).astype(bf16)
        a_ref[pl.ds(SUB * (width // LANES), META), :] = jnp.dot(
            meta_bf, back, preferred_element_type=f32).astype(bf16)
        for sub in range(4):
            put_sub(a_ref, b_ref, sub, ordered[SUB * sub:SUB * (sub + 1)], META)


def sub_place(sub, blocks, gap):
    return {0: (0, 0), 1: (1, 0), 2: (1, SUB * blocks), 3: (0, SUB * blocks + gap)}[sub]


def put_sub(a_ref, b_ref, sub, rows, gap):
    blocks = rows.shape[1] // LANES
    which, start = sub_place(sub, blocks, gap)
    ref = (a_ref, b_ref)[which]
    for c in range(blocks):
        ref[start + SUB * c:start + SUB * (c + 1), :] = rows[:, LANES * c:LANES * (c + 1)]


def get_block(refs, subs, blocks, gap, c):
    parts = []
    for sub in range(subs):
        which, start = sub_place(sub, blocks, gap)
        parts.append(refs[which][start + SUB * c:start + SUB * (c + 1), :])
    return parts[0] if subs == 1 else jnp.concatenate(parts, axis=0)


def expert_kernel(*refs, specs, steps):
    where_ref = refs[0]
    cursor = 1
    sources = []
    for subs, _ in specs:
        take = 2 if subs > 1 else 1
        sources.append(refs[cursor:cursor + take])
        cursor += take
    gates, ups, downs = refs[cursor:cursor + 2], refs[cursor + 2:cursor + 4], refs[cursor + 4:cursor + 6]
    cursor += 6
    results = []
    for subs, _ in specs:
        take = 2 if subs > 1 else 1
        results.append(refs[cursor:cursor + take])
        cursor += take
    rows_ref, sum_ref, hot_ref, factor_ref = refs[cursor:cursor + 4]
    width = rows_ref.shape[1]
    blocks = width // LANES
    step = pl.program_id(0)
    expert, parity = where_ref[0], where_ref[1]

    @pl.when(step == 0)
    def _():
        before = (iota((LANES, LANES), 0) < iota((LANES, LANES), 1)).astype(f32).astype(bf16)
        lane = iota((1, LANES), 1)
        for number, (subs, only) in enumerate(specs):
            meta = sources[number][0][SUB * blocks:SUB * blocks + META, :].astype(f32)
            target = expert.astype(f32)
            valid = lane < SUB * subs
            if only is not None:
                valid = valid & (lane < jnp.where(parity == only, LANES, 0))
            first = (meta[0:1] == target) & valid
            second = (meta[1:2] == target) & valid
            factor = jnp.where(first, (meta[2:3] + meta[3:4]) + meta[4:5], 0.0)
            factor = factor + jnp.where(second, (meta[5:6] + meta[6:7]) + meta[7:8], 0.0)
            match = jnp.where(first | second, 1.0, 0.0)
            slot = jnp.dot(jnp.broadcast_to(match, (16, LANES)).astype(bf16), before,
                           preferred_element_type=f32)[0:1]
            slot = jnp.where(match > 0.0, slot, -1.0)
            hot = (slot == iota((SUB, LANES), 0).astype(f32)).astype(f32)
            span = pl.ds(SUB * number, SUB)
            factor_ref[span, :] = jnp.broadcast_to(
                jnp.sum(hot * factor, axis=1, keepdims=True), (SUB, LANES))
            hot_ref[span, :] = hot
            hot = hot[:, :SUB * subs].astype(bf16)
            for c in range(blocks):
                rows_ref[span, LANES * c:LANES * (c + 1)] = jnp.dot(
                    hot, get_block(sources[number], subs, blocks, META, c),
                    preferred_element_type=f32).astype(bf16)

    rows = rows_ref[...]
    tile = gates[0].shape[2]
    actives = []
    for gate_ref, up_ref in zip(gates, ups):
        both = jnp.dot(rows, jnp.concatenate([gate_ref[0], up_ref[0]], axis=1),
                       preferred_element_type=f32)
        gate = jnp.minimum(both[:, :tile], clamp_limit)
        up = jnp.clip(both[:, tile:], -clamp_limit, clamp_limit)
        actives.append(((up + 1.0) * (gate * jax.nn.sigmoid(gate * sigmoid_slope))).astype(bf16))
    part = jnp.dot(jnp.concatenate(actives, axis=1),
                   jnp.concatenate([downs[0][0], downs[1][0]], axis=0),
                   preferred_element_type=f32)
    sum_ref[...] = jnp.where(step == 0, 0.0, sum_ref[...]) + part

    @pl.when(step == steps - 1)
    def _():
        for number, (subs, _) in enumerate(specs):
            span = pl.ds(SUB * number, SUB)
            weighted = (sum_ref[span, :] * factor_ref[span, 0:1]).astype(bf16)
            spread = hot_ref[span, :].T[:SUB * subs].astype(bf16)
            dense = jnp.dot(spread, weighted, preferred_element_type=f32).astype(bf16)
            pair = results[number]
            for sub in range(subs):
                put_sub(pair[0], pair[-1], sub, dense[SUB * sub:SUB * (sub + 1)], 0)


def finish_kernel(*refs):
    *messages, upt_ref, downt_ref, out_ref = refs
    width = out_ref.shape[1]
    blocks = width // LANES
    ways = ((upt_ref, messages[0:2]), (upt_ref, messages[2:4]), (downt_ref, messages[4:6]))
    for c in range(blocks):
        total = None
        for back_ref, pair in ways:
            part = jnp.dot(back_ref[...], get_block(pair, 4, blocks, 0, c), preferred_element_type=f32)
            total = part if total is None else total + part
        out_ref[:, LANES * c:LANES * (c + 1)] = total.astype(bf16)


VMEM = pl.BlockSpec(memory_space=pltpu.VMEM)
SMEM = pl.BlockSpec(memory_space=pltpu.SMEM)


def apply_experts(where, sources, specs, weights, partner_weights):
    width = weights[0].shape[1]
    hidden = weights[0].shape[2]
    tile = min(LANES, hidden)
    steps = hidden // tile
    blocks = width // LANES
    flat, out_shapes, in_specs, out_specs = [], [], [SMEM], []
    held = lambda shape: pl.BlockSpec(shape, lambda i: (0, 0), pipeline_mode=pl.Buffered(1))
    for (subs, _), pair in zip(specs, sources):
        flat += list(pair)
        in_specs += [held(x.shape) for x in pair]
        sizes = message_rows(subs, blocks)
        out_shapes += [jax.ShapeDtypeStruct((n, LANES), bf16) for n in sizes]
        out_specs += [held((n, LANES)) for n in sizes]
    in_specs += [pl.BlockSpec((1, width, tile), lambda i: (0, 0, i))] * 4
    in_specs += [pl.BlockSpec((1, tile, width), lambda i: (0, i, 0))] * 2
    rows = SUB * len(specs)
    outs = pl.pallas_call(
        partial(expert_kernel, specs=tuple(specs), steps=steps),
        grid=(steps,),
        in_specs=in_specs,
        out_specs=out_specs,
        out_shape=out_shapes,
        scratch_shapes=[pltpu.VMEM((rows, width), bf16), pltpu.VMEM((rows, width), f32),
                        pltpu.VMEM((rows, LANES), f32), pltpu.VMEM((rows, LANES), f32)],
        compiler_params=pltpu.CompilerParams(
            dimension_semantics=("arbitrary",), vmem_limit_bytes=56 * 1024 * 1024),
        cost_estimate=pl.CostEstimate(
            flops=6 * rows * width * 2 * hidden, transcendentals=0,
            bytes_accessed=12 * width * hidden),
        interpret=INTERPRET,
        name="experts",
    )(where, *flat, weights[0], partner_weights[0], weights[1], partner_weights[1],
      weights[2], partner_weights[2])
    results, cursor = [], 0
    for subs, _ in specs:
        take = len(message_rows(subs, blocks))
        results.append(list(outs[cursor:cursor + take]))
        cursor += take
    return results


def message_rows(subs, blocks):
    first = SUB * blocks * (2 if subs == 4 else 1)
    second = SUB * blocks * min(subs - 1, 2)
    return [first, second] if second else [first]


def layer(tokens, norm_gain, expert_ids, route_weight, gate_weight, up_weight, down_weight):
    devices = lax.axis_size("ep")
    ring = devices // 2
    experts = ring // 2
    rows, width = tokens.shape
    blocks = width // LANES
    capacity = min(rows, 2 * rows * expert_ids.shape[1] // experts)
    hops = ring // 2
    chip = lax.axis_index("ep") // 2
    where = jnp.stack([chip // 2, chip % 2]).astype(jnp.int32)
    subs_at = [4] + [
        min(rows, capacity * (experts // 2 - (k + 1) // 2 + 1)) // SUB for k in range(1, hops + 1)]

    swap = [(i, i ^ 1) for i in range(devices)]
    weights = (gate_weight, up_weight, down_weight)
    partner = tuple(lax.ppermute(w, "ep", swap) for w in weights)

    full = message_rows(4, blocks)
    shapes = [jax.ShapeDtypeStruct((full[0] + META, LANES), bf16),
              jax.ShapeDtypeStruct((full[1], LANES), bf16)]
    upa, upb, downa, downb, up_back, down_back = pl.pallas_call(
        partial(prepare_kernel, experts=experts),
        in_specs=[SMEM, VMEM, VMEM, VMEM, VMEM],
        out_specs=[VMEM] * 6,
        out_shape=shapes * 2 + [jax.ShapeDtypeStruct((rows, rows), bf16)] * 2,
        interpret=INTERPRET,
        name="prepare",
    )(where, tokens, norm_gain.reshape(1, width), expert_ids, route_weight)

    def cut(pair, subs, gap):
        sizes = message_rows(subs, blocks)
        if gap:
            sizes[0] += META
        return [x[:n] if x.shape[0] != n else x for x, n in zip(pair, sizes)]

    arrived = {(0, 0): [upa, upb]}
    moving = {1: [upa, upb], -1: [downa, downb]}
    for k in range(1, hops + 1):
        for way in (1, -1):
            moving[way] = [shifted(x, 2 * way)
                           for x in cut(moving[way], subs_at[k], True)]
            arrived[way, k] = moving[way]

    given = {}
    for low in range(0, hops, STRIDE):
        keys = [(0, 0)] if low == 0 else []
        keys += [(way, k) for k in range(low + 1, low + STRIDE + 1) for way in (1, -1)]
        specs = [(subs_at[k], None if k < hops else (1 if way == 1 else 0)) for way, k in keys]
        values = apply_experts(where, [arrived[k] for k in keys], specs, weights, partner)
        given.update(zip(keys, values))

    totals = {way: given[way, hops] for way in (1, -1)}
    for k in range(hops - 1, -1, -1):
        for way in (1, -1):
            came = [shifted(x, -2 * way)
                    for x in totals[way]]
            if k == 0:
                totals[way] = came
                continue
            mine = given[way, k]
            joined = []
            for number, value in enumerate(mine):
                if number < len(came):
                    more = came[number]
                    padded = jnp.pad(more, ((0, value.shape[0] - more.shape[0]), (0, 0)))
                    value = (value.astype(f32) + padded.astype(f32)).astype(bf16)
                joined.append(value)
            totals[way] = joined

    return pl.pallas_call(
        finish_kernel,
        in_specs=[VMEM] * 8,
        out_specs=VMEM,
        out_shape=jax.ShapeDtypeStruct((rows, width), bf16),
        interpret=INTERPRET,
        name="finish",
    )(*given[0, 0], *totals[1], *totals[-1], up_back, down_back)


def solution(mesh):
    placed = (
        P(("grp", "ep"), None),
        P(),
        P(("grp", "ep"), None),
        P(("grp", "ep"), None),
        P("ep", None, None),
        P("ep", None, None),
        P("ep", None, None),
    )
    return jax.shard_map(
        layer, mesh=mesh, in_specs=placed, out_specs=P(("grp", "ep"), None), check_vma=False
    )
```

```python
from functools import partial

import jax
import jax.numpy as jnp
from jax import lax
from jax.experimental import pallas as pl
from jax.experimental.pallas import tpu as pltpu
from jax.sharding import PartitionSpec as P


INTERPRET = False
LANES = 128
SUB = 32
LIMIT = 24 * 1024 * 1024
STRIDE = 2
META = 16
EPSILON = 1e-05
clamp_limit = 7.0
sigmoid_slope = 1.702
f32 = jnp.float32
bf16 = jnp.bfloat16


def shifted(array, step):
    size = lax.axis_size("ep")
    return lax.ppermute(array, "ep", [(i, (i + step) % size) for i in range(size)])


def iota(shape, axis):
    return lax.broadcasted_iota(jnp.int32, shape, axis)


def reaches(ids, pair, parity, experts):
    half = experts // 2
    ahead = ids - pair
    ahead = jnp.where(ahead < 0, ahead + experts, ahead)
    behind = experts - ahead
    up_even = jnp.where(ahead < half, 2 * ahead + 1, 0)
    up_odd = jnp.where((ahead >= 1) & (ahead <= half), 2 * ahead, 0)
    down_even = jnp.where(ahead >= half, 2 * behind, 0)
    down_odd = jnp.where(ahead == 0, 1, jnp.where(ahead > half, 2 * behind + 1, 0))
    even = parity == 0
    return jnp.where(even, up_even, up_odd), jnp.where(even, down_even, down_odd)


def prepare_kernel(where_ref, tokens_ref, gain_ref, ids_ref, weight_ref,
                   upa_ref, upb_ref, downa_ref, downb_ref, upt_ref, downt_ref, *, experts):
    rows, width = tokens_ref.shape
    pair, parity = where_ref[0], where_ref[1]
    values = tokens_ref[...].astype(f32)
    center = values - jnp.mean(values, axis=-1, keepdims=True)
    spread = jnp.mean(center * center, axis=-1, keepdims=True)
    normed = (center * lax.rsqrt(spread + EPSILON) * gain_ref[...]).astype(bf16)

    weights = weight_ref[...]
    high = weights.astype(bf16).astype(f32)
    middle = (weights - high).astype(bf16).astype(f32)
    low = weights - high - middle
    sub = iota((rows, rows), 0)
    meta = jnp.zeros((rows, rows), f32)
    entries = [ids_ref[0:1, :].astype(f32), ids_ref[1:2, :].astype(f32)]
    for k in range(2):
        entries += [high[k:k + 1, :], middle[k:k + 1, :], low[k:k + 1, :]]
    for number, entry in enumerate(entries):
        meta = jnp.where(sub == number, entry, meta)
    table = meta.T
    meta_bf = meta[0:META, :].astype(bf16)
    first_c, second_c = table[:, 0:1].astype(jnp.int32), table[:, 1:2].astype(jnp.int32)
    first_r, second_r = ids_ref[0:1, :], ids_ref[1:2, :]
    reach_c = [jnp.maximum(a, b) for a, b in zip(
        reaches(first_c, pair, parity, experts), reaches(second_c, pair, parity, experts))]
    reach_r = [jnp.maximum(a, b) for a, b in zip(
        reaches(first_r, pair, parity, experts), reaches(second_r, pair, parity, experts))]
    sub_i, lane_i = iota((rows, rows), 0), iota((rows, rows), 1)
    for way, (a_ref, b_ref, t_ref) in enumerate(
            ((upa_ref, upb_ref, upt_ref), (downa_ref, downb_ref, downt_ref))):
        col, row = reach_c[way], reach_r[way]
        ahead_c = (row > col) | ((row == col) & (lane_i < sub_i))
        ahead_r = (col > row) | ((col == row) & (sub_i < lane_i))
        rank_c = jnp.sum(ahead_c.astype(f32), axis=1, keepdims=True).astype(jnp.int32)
        rank_r = jnp.sum(ahead_r.astype(f32), axis=0, keepdims=True).astype(jnp.int32)
        back = (rank_c == lane_i).astype(f32).astype(bf16)
        order = (rank_r == sub_i).astype(f32).astype(bf16)
        t_ref[...] = back
        ordered = jnp.dot(order, normed, preferred_element_type=f32).astype(bf16)
        a_ref[pl.ds(SUB * (width // LANES), META), :] = jnp.dot(
            meta_bf, back, preferred_element_type=f32).astype(bf16)
        for sub in range(4):
            put_sub(a_ref, b_ref, sub, ordered[SUB * sub:SUB * (sub + 1)], META)


def sub_place(sub, blocks, gap):
    return {0: (0, 0), 1: (1, 0), 2: (1, SUB * blocks), 3: (0, SUB * blocks + gap)}[sub]


def put_sub(a_ref, b_ref, sub, rows, gap):
    blocks = rows.shape[1] // LANES
    which, start = sub_place(sub, blocks, gap)
    ref = (a_ref, b_ref)[which]
    for c in range(blocks):
        ref[start + SUB * c:start + SUB * (c + 1), :] = rows[:, LANES * c:LANES * (c + 1)]


def get_block(refs, subs, blocks, gap, c):
    parts = []
    for sub in range(subs):
        which, start = sub_place(sub, blocks, gap)
        parts.append(refs[which][start + SUB * c:start + SUB * (c + 1), :])
    return parts[0] if subs == 1 else jnp.concatenate(parts, axis=0)


def expert_kernel(*refs, specs):
    where_ref = refs[0]
    cursor = 1
    sources = []
    for subs, _ in specs:
        take = 2 if subs > 1 else 1
        sources.append(refs[cursor:cursor + take])
        cursor += take
    gate_ref, up_ref, down_ref = refs[cursor:cursor + 3]
    cursor += 3
    results = []
    for subs, _ in specs:
        take = 2 if subs > 1 else 1
        results.append(refs[cursor:cursor + take])
        cursor += take
    rows_ref, sum_ref, hot_ref, factor_ref = refs[cursor:cursor + 4]
    width = rows_ref.shape[1]
    blocks = width // LANES
    expert, parity = where_ref[0], where_ref[1]

    before = (iota((LANES, LANES), 0) < iota((LANES, LANES), 1)).astype(f32).astype(bf16)
    lane = iota((1, LANES), 1)
    for number, (subs, only) in enumerate(specs):
        meta = sources[number][0][SUB * blocks:SUB * blocks + META, :].astype(f32)
        target = expert.astype(f32)
        valid = lane < SUB * subs
        if only is not None:
            valid = valid & (lane < jnp.where(parity == only, LANES, 0))
        first = (meta[0:1] == target) & valid
        second = (meta[1:2] == target) & valid
        factor = jnp.where(first, (meta[2:3] + meta[3:4]) + meta[4:5], 0.0)
        factor = factor + jnp.where(second, (meta[5:6] + meta[6:7]) + meta[7:8], 0.0)
        match = jnp.where(first | second, 1.0, 0.0)
        slot = jnp.dot(jnp.broadcast_to(match, (16, LANES)).astype(bf16), before,
                       preferred_element_type=f32)[0:1]
        slot = jnp.where(match > 0.0, slot, -1.0)
        hot = (slot == iota((SUB, LANES), 0).astype(f32)).astype(f32)
        span = pl.ds(SUB * number, SUB)
        factor_ref[span, :] = jnp.broadcast_to(
            jnp.sum(hot * factor, axis=1, keepdims=True), (SUB, LANES))
        hot_ref[span, :] = hot
        hot = hot[:, :SUB * subs].astype(bf16)
        for c in range(blocks):
            rows_ref[span, LANES * c:LANES * (c + 1)] = jnp.dot(
                hot, get_block(sources[number], subs, blocks, META, c),
                preferred_element_type=f32).astype(bf16)

    hidden = gate_ref.shape[1]
    tile = min(256, hidden)

    def add_tile(number, _):
        span = pl.ds(pl.multiple_of(number * tile, tile), tile)
        rows = rows_ref[...]
        gate = jnp.minimum(jnp.dot(rows, gate_ref[:, span], preferred_element_type=f32), clamp_limit)
        up = jnp.clip(jnp.dot(rows, up_ref[:, span], preferred_element_type=f32),
                      -clamp_limit, clamp_limit)
        active = ((up + 1.0) * (gate * jax.nn.sigmoid(gate * sigmoid_slope))).astype(bf16)
        part = jnp.dot(active, down_ref[span, :], preferred_element_type=f32)
        sum_ref[...] = jnp.where(number == 0, 0.0, sum_ref[...]) + part
        return 0

    lax.fori_loop(0, hidden // tile, add_tile, 0)

    for number, (subs, _) in enumerate(specs):
        span = pl.ds(SUB * number, SUB)
        weighted = (sum_ref[span, :] * factor_ref[span, 0:1]).astype(bf16)
        spread = hot_ref[span, :].T[:SUB * subs].astype(bf16)
        dense = jnp.dot(spread, weighted, preferred_element_type=f32).astype(bf16)
        pair = results[number]
        for sub in range(subs):
            put_sub(pair[0], pair[-1], sub, dense[SUB * sub:SUB * (sub + 1)], 0)


def finish_kernel(*refs):
    *messages, upt_ref, downt_ref, out_ref = refs
    width = out_ref.shape[1]
    blocks = width // LANES
    ways = ((upt_ref, messages[0:2]), (upt_ref, messages[2:4]), (downt_ref, messages[4:6]))
    for c in range(blocks):
        total = None
        for back_ref, pair in ways:
            part = jnp.dot(back_ref[...], get_block(pair, 4, blocks, 0, c), preferred_element_type=f32)
            total = part if total is None else total + part
        out_ref[:, LANES * c:LANES * (c + 1)] = total.astype(bf16)


VMEM = pl.BlockSpec(memory_space=pltpu.VMEM)
SMEM = pl.BlockSpec(memory_space=pltpu.SMEM)


def hold_kernel(*refs):
    for n in range(2):
        hidden = refs[2 * n].shape[2]
        refs[6 + n][:, :hidden] = refs[2 * n][0]
        refs[6 + n][:, hidden:] = refs[2 * n + 1][0]
    hidden = refs[4].shape[1]
    refs[8][:hidden, :] = refs[4][0]
    refs[8][hidden:, :] = refs[5][0]


def hold_weights(weights, partner):
    _, width, hidden = weights[0].shape
    shapes = [(width, 2 * hidden)] * 2 + [(2 * hidden, width)]
    return pl.pallas_call(
        hold_kernel,
        in_specs=[VMEM] * 6,
        out_specs=[VMEM] * 3,
        out_shape=[pltpu.VMEM(shape, bf16) for shape in shapes],
        compiler_params=pltpu.CompilerParams(vmem_limit_bytes=28 * 1024 * 1024),
        interpret=INTERPRET,
        name="hold",
    )(weights[0], partner[0], weights[1], partner[1], weights[2], partner[2])


def apply_experts(where, sources, specs, weights):
    width, hidden = weights[0].shape
    blocks = width // LANES
    flat, out_shapes, in_specs, out_specs = [], [], [SMEM], []
    for (subs, _), pair in zip(specs, sources):
        flat += list(pair)
        in_specs += [VMEM] * len(pair)
        sizes = message_rows(subs, blocks)
        out_shapes += [jax.ShapeDtypeStruct((n, LANES), bf16) for n in sizes]
        out_specs += [VMEM] * len(sizes)
    in_specs += [VMEM] * 3
    rows = SUB * len(specs)
    outs = pl.pallas_call(
        partial(expert_kernel, specs=tuple(specs)),
        in_specs=in_specs,
        out_specs=out_specs,
        out_shape=out_shapes,
        scratch_shapes=[pltpu.VMEM((rows, width), bf16), pltpu.VMEM((rows, width), f32),
                        pltpu.VMEM((rows, LANES), f32), pltpu.VMEM((rows, LANES), f32)],
        compiler_params=pltpu.CompilerParams(vmem_limit_bytes=LIMIT),
        cost_estimate=pl.CostEstimate(
            flops=6 * rows * width * hidden, transcendentals=0,
            bytes_accessed=6 * width * hidden),
        interpret=INTERPRET,
        name="experts",
    )(where, *flat, *weights)
    results, cursor = [], 0
    for subs, _ in specs:
        take = len(message_rows(subs, blocks))
        results.append(list(outs[cursor:cursor + take]))
        cursor += take
    return results


def message_rows(subs, blocks):
    first = SUB * blocks * (2 if subs == 4 else 1)
    second = SUB * blocks * min(subs - 1, 2)
    return [first, second] if second else [first]


def layer(tokens, norm_gain, expert_ids, route_weight, gate_weight, up_weight, down_weight):
    devices = lax.axis_size("ep")
    ring = devices // 2
    experts = ring // 2
    rows, width = tokens.shape
    blocks = width // LANES
    capacity = min(rows, 2 * rows * expert_ids.shape[1] // experts)
    hops = ring // 2
    chip = lax.axis_index("ep") // 2
    where = jnp.stack([chip // 2, chip % 2]).astype(jnp.int32)
    subs_at = [4] + [
        min(rows, capacity * (experts // 2 - (k + 1) // 2 + 1)) // SUB for k in range(1, hops + 1)]

    swap = [(i, i ^ 1) for i in range(devices)]
    weights = (gate_weight, up_weight, down_weight)
    partner = tuple(lax.ppermute(w, "ep", swap) for w in weights)

    held = hold_weights(weights, partner)

    full = message_rows(4, blocks)
    shapes = [jax.ShapeDtypeStruct((full[0] + META, LANES), bf16),
              jax.ShapeDtypeStruct((full[1], LANES), bf16)]
    upa, upb, downa, downb, up_back, down_back = pl.pallas_call(
        partial(prepare_kernel, experts=experts),
        in_specs=[SMEM, VMEM, VMEM, VMEM, VMEM],
        out_specs=[VMEM] * 6,
        out_shape=shapes * 2 + [jax.ShapeDtypeStruct((rows, rows), bf16)] * 2,
        interpret=INTERPRET,
        name="prepare",
    )(where, tokens, norm_gain.reshape(1, width), expert_ids.T, route_weight.T)

    def cut(pair, subs, gap):
        sizes = message_rows(subs, blocks)
        if gap:
            sizes[0] += META
        return [x[:n] if x.shape[0] != n else x for x, n in zip(pair, sizes)]

    arrived = {(0, 0): [upa, upb]}
    moving = {1: [upa, upb], -1: [downa, downb]}
    for k in range(1, hops + 1):
        for way in (1, -1):
            moving[way] = [shifted(x, 2 * way)
                           for x in cut(moving[way], subs_at[k], True)]
            arrived[way, k] = moving[way]

    given = {}
    for low in range(0, hops, STRIDE):
        keys = [(0, 0)] if low == 0 else []
        keys += [(way, k) for k in range(low + 1, low + STRIDE + 1) for way in (1, -1)]
        specs = [(subs_at[k], None if k < hops else (1 if way == 1 else 0)) for way, k in keys]
        values = apply_experts(where, [arrived[k] for k in keys], specs, held)
        given.update(zip(keys, values))

    totals = {way: given[way, hops] for way in (1, -1)}
    for k in range(hops - 1, -1, -1):
        for way in (1, -1):
            came = [shifted(x, -2 * way)
                    for x in totals[way]]
            if k == 0:
                totals[way] = came
                continue
            mine = given[way, k]
            joined = []
            for number, value in enumerate(mine):
                if number < len(came):
                    more = came[number]
                    padded = jnp.pad(more, ((0, value.shape[0] - more.shape[0]), (0, 0)))
                    value = (value.astype(f32) + padded.astype(f32)).astype(bf16)
                joined.append(value)
            totals[way] = joined

    return pl.pallas_call(
        finish_kernel,
        in_specs=[VMEM] * 8,
        out_specs=VMEM,
        out_shape=jax.ShapeDtypeStruct((rows, width), bf16),
        interpret=INTERPRET,
        name="finish",
    )(*given[0, 0], *totals[1], *totals[-1], up_back, down_back)


def solution(mesh):
    placed = (
        P(("grp", "ep"), None),
        P(),
        P(("grp", "ep"), None),
        P(("grp", "ep"), None),
        P("ep", None, None),
        P("ep", None, None),
        P("ep", None, None),
    )
    return jax.shard_map(
        layer, mesh=mesh, in_specs=placed, out_specs=P(("grp", "ep"), None), check_vma=False
    )
```

```python
from functools import partial

import jax
import jax.numpy as jnp
from jax import lax
from jax.experimental import pallas as pl
from jax.experimental.pallas import tpu as pltpu
from jax.sharding import PartitionSpec as P


INTERPRET = False
LANES = 128
SUB = 32
LIMIT = 24 * 1024 * 1024
RUNS = 4
META = 16
EPSILON = 1e-05
clamp_limit = 7.0
sigmoid_slope = 1.702
f32 = jnp.float32
bf16 = jnp.bfloat16


def shifted(array, step):
    size = lax.axis_size("ep")
    return lax.ppermute(array, "ep", [(i, (i + step) % size) for i in range(size)])


def iota(shape, axis):
    return lax.broadcasted_iota(jnp.int32, shape, axis)


def reaches(ids, pair, parity, experts):
    half = experts // 2
    ahead = ids - pair
    ahead = jnp.where(ahead < 0, ahead + experts, ahead)
    behind = experts - ahead
    up_even = jnp.where(ahead < half, 2 * ahead + 1, 0)
    up_odd = jnp.where((ahead >= 1) & (ahead <= half), 2 * ahead, 0)
    down_even = jnp.where(ahead >= half, 2 * behind, 0)
    down_odd = jnp.where(ahead == 0, 1, jnp.where(ahead > half, 2 * behind + 1, 0))
    even = parity == 0
    return jnp.where(even, up_even, up_odd), jnp.where(even, down_even, down_odd)


def prepare_kernel(where_ref, tokens_ref, gain_ref, ids_ref, weight_ref,
                   *out_refs, experts):
    rows, width = tokens_ref.shape
    pair, parity = where_ref[0], where_ref[1]
    values = tokens_ref[...].astype(f32)
    center = values - jnp.mean(values, axis=-1, keepdims=True)
    spread = jnp.mean(center * center, axis=-1, keepdims=True)
    normed = (center * lax.rsqrt(spread + EPSILON) * gain_ref[...]).astype(bf16)

    weights = weight_ref[...]
    high = weights.astype(bf16).astype(f32)
    middle = (weights - high).astype(bf16).astype(f32)
    low = weights - high - middle
    sub = iota((rows, rows), 0)
    meta = jnp.zeros((rows, rows), f32)
    entries = [ids_ref[0:1, :].astype(f32), ids_ref[1:2, :].astype(f32)]
    for k in range(2):
        entries += [high[k:k + 1, :], middle[k:k + 1, :], low[k:k + 1, :]]
    for number, entry in enumerate(entries):
        meta = jnp.where(sub == number, entry, meta)
    table = meta.T
    meta_bf = meta[0:META, :].astype(bf16)
    first_c, second_c = table[:, 0:1].astype(jnp.int32), table[:, 1:2].astype(jnp.int32)
    first_r, second_r = ids_ref[0:1, :], ids_ref[1:2, :]
    reach_c = [jnp.maximum(a, b) for a, b in zip(
        reaches(first_c, pair, parity, experts), reaches(second_c, pair, parity, experts))]
    reach_r = [jnp.maximum(a, b) for a, b in zip(
        reaches(first_r, pair, parity, experts), reaches(second_r, pair, parity, experts))]
    sub_i, lane_i = iota((rows, rows), 0), iota((rows, rows), 1)
    blocks = width // LANES
    for way in range(2):
        run_refs, t_ref = out_refs[RUNS * way:RUNS * (way + 1)], out_refs[2 * RUNS + way]
        col, row = reach_c[way], reach_r[way]
        ahead_c = (row > col) | ((row == col) & (lane_i < sub_i))
        ahead_r = (col > row) | ((col == row) & (sub_i < lane_i))
        rank_c = jnp.sum(ahead_c.astype(f32), axis=1, keepdims=True).astype(jnp.int32)
        rank_r = jnp.sum(ahead_r.astype(f32), axis=0, keepdims=True).astype(jnp.int32)
        back = (rank_c == lane_i).astype(f32).astype(bf16)
        order = (rank_r == sub_i).astype(f32).astype(bf16)
        t_ref[...] = back
        ordered = jnp.dot(order, normed, preferred_element_type=f32).astype(bf16)
        run_refs[0][SUB * blocks:SUB * blocks + META, :] = jnp.dot(
            meta_bf, back, preferred_element_type=f32).astype(bf16)
        for run in range(RUNS):
            put_run(run_refs[run], ordered[SUB * run:SUB * (run + 1)])


def put_run(ref, rows):
    for c in range(rows.shape[1] // LANES):
        ref[SUB * c:SUB * (c + 1), :] = rows[:, LANES * c:LANES * (c + 1)]


def get_block(refs, places, c):
    parts = [refs[n][start + SUB * c:start + SUB * (c + 1), :] for n, start in places]
    return parts[0] if len(parts) == 1 else jnp.concatenate(parts, axis=0)


def expert_kernel(*refs, specs, count):
    where_ref = refs[0]
    sources = refs[1:1 + count]
    gate_ref, up_ref, down_ref = refs[1 + count:4 + count]
    results = refs[4 + count:-4]
    rows_ref, sum_ref, hot_ref, factor_ref = refs[-4:]
    width = rows_ref.shape[1]
    blocks = width // LANES
    expert, parity = where_ref[0], where_ref[1]

    before = (iota((LANES, LANES), 0) < iota((LANES, LANES), 1)).astype(f32).astype(bf16)
    lane = iota((1, LANES), 1)
    for number, (places, only) in enumerate(specs):
        index, start = places[0]
        start = start + SUB * blocks
        meta = sources[index][start:start + META, :].astype(f32)
        target = expert.astype(f32)
        valid = lane < SUB * len(places)
        if only is not None:
            valid = valid & (lane < jnp.where(parity == only, LANES, 0))
        first = (meta[0:1] == target) & valid
        second = (meta[1:2] == target) & valid
        factor = jnp.where(first, (meta[2:3] + meta[3:4]) + meta[4:5], 0.0)
        factor = factor + jnp.where(second, (meta[5:6] + meta[6:7]) + meta[7:8], 0.0)
        match = jnp.where(first | second, 1.0, 0.0)
        slot = jnp.dot(jnp.broadcast_to(match, (16, LANES)).astype(bf16), before,
                       preferred_element_type=f32)[0:1]
        slot = jnp.where(match > 0.0, slot, -1.0)
        hot = (slot == iota((SUB, LANES), 0).astype(f32)).astype(f32)
        span = pl.ds(SUB * number, SUB)
        factor_ref[span, :] = jnp.broadcast_to(
            jnp.sum(hot * factor, axis=1, keepdims=True), (SUB, LANES))
        hot_ref[span, :] = hot
        hot = hot[:, :SUB * len(places)].astype(bf16)
        for c in range(blocks):
            rows_ref[span, LANES * c:LANES * (c + 1)] = jnp.dot(
                hot, get_block(sources, places, c), preferred_element_type=f32).astype(bf16)

    hidden = gate_ref.shape[1]
    tile = min(256, hidden)

    def add_tile(number, _):
        span = pl.ds(pl.multiple_of(number * tile, tile), tile)
        rows = rows_ref[...]
        gate = jnp.minimum(jnp.dot(rows, gate_ref[:, span], preferred_element_type=f32), clamp_limit)
        up = jnp.clip(jnp.dot(rows, up_ref[:, span], preferred_element_type=f32),
                      -clamp_limit, clamp_limit)
        active = ((up + 1.0) * (gate * jax.nn.sigmoid(gate * sigmoid_slope))).astype(bf16)
        part = jnp.dot(active, down_ref[span, :], preferred_element_type=f32)
        sum_ref[...] = jnp.where(number == 0, 0.0, sum_ref[...]) + part
        return 0

    lax.fori_loop(0, hidden // tile, add_tile, 0)

    cursor = 0
    for number, (places, _) in enumerate(specs):
        span = pl.ds(SUB * number, SUB)
        weighted = (sum_ref[span, :] * factor_ref[span, 0:1]).astype(bf16)
        spread = hot_ref[span, :].T[:SUB * len(places)].astype(bf16)
        dense = jnp.dot(spread, weighted, preferred_element_type=f32).astype(bf16)
        for run in range(len(places)):
            put_run(results[cursor], dense[SUB * run:SUB * (run + 1)])
            cursor += 1


def join_kernel(*refs, parts):
    *in_refs, out_ref = refs
    size = out_ref.shape[0] // len(parts)
    cursor = 1 if any(came is not None for came, _ in parts) else 0
    for number, (came, adds) in enumerate(parts):
        mine = None
        if adds:
            mine = in_refs[cursor]
            cursor += 1

        def step(i, _, number=number, came=came, mine=mine):
            total = 0.0
            at = pl.multiple_of(i * 64, 64)
            if came is not None:
                total = in_refs[0][pl.ds(came + at, 64), :].astype(f32)
            if mine is not None:
                total = total + mine[pl.ds(at, 64), :].astype(f32)
            out_ref[pl.ds(number * size + at, 64), :] = total.astype(bf16)
            return 0

        lax.fori_loop(0, size // 64, step, 0)


def join(came, parts):
    size = next(mine for _, mine in parts).shape[0]
    operands = ([] if came is None else [came]) + [mine for _, mine in parts if mine is not None]
    spec = tuple((start, mine is not None) for start, mine in parts)
    if came is not None and all(start is None for start, _ in parts):
        operands = operands[1:]
    return pl.pallas_call(
        partial(join_kernel, parts=spec),
        in_specs=[VMEM] * len(operands),
        out_specs=VMEM,
        out_shape=jax.ShapeDtypeStruct((size * len(parts), LANES), bf16),
        compiler_params=pltpu.CompilerParams(vmem_limit_bytes=4 * 1024 * 1024),
        interpret=INTERPRET,
        name="join",
    )(*operands)


def finish_kernel(*refs, specs):
    *in_refs, upt_ref, downt_ref, out_ref = refs
    blocks = out_ref.shape[1] // LANES
    for c in range(blocks):
        total = None
        for back_ref, places in zip((upt_ref, upt_ref, downt_ref), specs):
            part = jnp.dot(back_ref[...], get_block(in_refs, places, c), preferred_element_type=f32)
            total = part if total is None else total + part
        out_ref[:, LANES * c:LANES * (c + 1)] = total.astype(bf16)


VMEM = pl.BlockSpec(memory_space=pltpu.VMEM)
SMEM = pl.BlockSpec(memory_space=pltpu.SMEM)


def hold_kernel(*refs):
    for n in range(2):
        hidden = refs[2 * n].shape[2]
        refs[6 + n][:, :hidden] = refs[2 * n][0]
        refs[6 + n][:, hidden:] = refs[2 * n + 1][0]
    hidden = refs[4].shape[1]
    refs[8][:hidden, :] = refs[4][0]
    refs[8][hidden:, :] = refs[5][0]


def hold_weights(weights, partner):
    _, width, hidden = weights[0].shape
    shapes = [(width, 2 * hidden)] * 2 + [(2 * hidden, width)]
    return pl.pallas_call(
        hold_kernel,
        in_specs=[VMEM] * 6,
        out_specs=[VMEM] * 3,
        out_shape=[pltpu.VMEM(shape, bf16) for shape in shapes],
        compiler_params=pltpu.CompilerParams(vmem_limit_bytes=28 * 1024 * 1024),
        interpret=INTERPRET,
        name="hold",
    )(weights[0], partner[0], weights[1], partner[1], weights[2], partner[2])


def gathered(pieces):
    arrays, specs = [], []
    for places in pieces:
        numbers = []
        for array, start in places:
            found = [n for n, a in enumerate(arrays) if a is array]
            if not found:
                arrays.append(array)
            numbers.append((found[0] if found else len(arrays) - 1, start))
        specs.append(tuple(numbers))
    return arrays, tuple(specs)


def apply_experts(where, pieces, parities, weights):
    width, hidden = weights[0].shape
    arrays, places = gathered(pieces)
    runs = sum(len(p) for p in places)
    rows = SUB * len(places)
    outs = pl.pallas_call(
        partial(expert_kernel, specs=tuple(zip(places, parities)), count=len(arrays)),
        in_specs=[SMEM] + [VMEM] * (len(arrays) + 3),
        out_specs=[VMEM] * runs,
        out_shape=[jax.ShapeDtypeStruct((SUB * width // LANES, LANES), bf16)] * runs,
        scratch_shapes=[pltpu.VMEM((rows, width), bf16), pltpu.VMEM((rows, width), f32),
                        pltpu.VMEM((rows, LANES), f32), pltpu.VMEM((rows, LANES), f32)],
        compiler_params=pltpu.CompilerParams(vmem_limit_bytes=LIMIT),
        cost_estimate=pl.CostEstimate(
            flops=6 * rows * width * hidden, transcendentals=0,
            bytes_accessed=6 * width * hidden),
        interpret=INTERPRET,
        name="experts",
    )(where, *arrays, *weights)
    results, cursor = [], 0
    for p in places:
        results.append(list(outs[cursor:cursor + len(p)]))
        cursor += len(p)
    return results


def layer(tokens, norm_gain, expert_ids, route_weight, gate_weight, up_weight, down_weight):
    devices = lax.axis_size("ep")
    ring = devices // 2
    experts = ring // 2
    rows, width = tokens.shape
    blocks = width // LANES
    capacity = min(rows, 2 * rows * expert_ids.shape[1] // experts)
    hops = ring // 2
    chip = lax.axis_index("ep") // 2
    where = jnp.stack([chip // 2, chip % 2]).astype(jnp.int32)
    reach, lag, ready = plan(hops, capacity, rows)

    swap = [(i, i ^ 1) for i in range(devices)]
    weights = (gate_weight, up_weight, down_weight)
    partner = []
    for w in weights:
        partner.append(lax.ppermute(w, "ep", swap))

    held = hold_weights(weights, partner)

    size = SUB * blocks
    shapes = [jax.ShapeDtypeStruct((size + META, LANES), bf16)]
    shapes += [jax.ShapeDtypeStruct((size, LANES), bf16)] * (RUNS - 1)
    outs = pl.pallas_call(
        partial(prepare_kernel, experts=experts),
        in_specs=[SMEM, VMEM, VMEM, VMEM, VMEM],
        out_specs=[VMEM] * (2 * RUNS + 2),
        out_shape=shapes * 2 + [jax.ShapeDtypeStruct((rows, rows), bf16)] * 2,
        interpret=INTERPRET,
        name="prepare",
    )(where, tokens, norm_gain.reshape(1, width), expert_ids.T, route_weight.T)
    mine = {1: outs[:RUNS], -1: outs[RUNS:2 * RUNS]}
    backs = outs[2 * RUNS:]

    arrived = {(0, 0): [(x, 0) for x in mine[1]]}
    moving = {way: [mine[way][0], mine[way][1]] for way in (1, -1)}
    for turn in range(1, hops + 1):
        for way in (1, -1):
            first, second = moving[way]
            if turn == lag[3] + 1:
                first = jnp.concatenate([first, mine[way][3]], axis=0)
            if turn == lag[2] + 1:
                second = jnp.concatenate([second, mine[way][2]], axis=0)
            if turn == reach[1] + 1:
                second = second[size:]
            first = shifted(first, 2 * way)
            second = shifted(second, 2 * way)
            moving[way] = [first, second]
            starts = [(first, 0), (second, 0),
                      (second, size if turn <= reach[1] else 0), (first, size + META)]
            for run in range(RUNS):
                k = turn - lag[run]
                if 1 <= k <= reach[run]:
                    arrived.setdefault((way, k), [None] * RUNS)[run] = starts[run]

    given = {}
    for _, distances in batches(hops, ready):
        keys = [(way, k) if k else (0, 0) for k in distances for way in ((1, -1) if k else (1,))]
        pieces = [[p for p in arrived[key] if p is not None] for key in keys]
        parities = [None if k < hops else (1 if way == 1 else 0) for way, k in keys]
        values = apply_experts(where, pieces, parities, held)
        given.update(zip(keys, values))

    final = {way: [None] * RUNS for way in (1, -1)}
    moving = {way: [None, None] for way in (1, -1)}
    came_at = {way: {} for way in (1, -1)}
    for turn in range(1, hops + 1):
        for way in (1, -1):
            for message, runs in enumerate(((0, 3), (1, 2))):
                parts, names = [], []
                for run in runs:
                    k = hops + 1 - lag[run] - turn
                    if 1 <= k <= reach[run]:
                        parts.append((came_at[way].get(run), given[way, k][run]))
                        names.append(run)
                sent = join(moving[way][message], parts)
                came = shifted(sent, -2 * way)
                moving[way][message] = came
                for position, run in enumerate(names):
                    came_at[way][run] = position * size
                    if hops - lag[run] - turn == 0:
                        final[way][run] = (came, position * size)

    arrays, places = gathered([[(x, 0) for x in given[0, 0]], final[1], final[-1]])
    return pl.pallas_call(
        partial(finish_kernel, specs=places),
        in_specs=[VMEM] * (len(arrays) + 2),
        out_specs=VMEM,
        out_shape=jax.ShapeDtypeStruct((rows, width), bf16),
        interpret=INTERPRET,
        name="finish",
    )(*arrays, *backs)


def plan(hops, capacity, rows):
    reach = []
    for run in range(RUNS):
        reach.append(max(k for k in range(1, hops + 1)
                         if min(rows, capacity * (hops // 2 - (k + 1) // 2 + 1)) > SUB * run))
    lag = [0, 0, hops - reach[2], hops - reach[3]]
    ready = {k: max(k + lag[run] for run in range(RUNS) if k <= reach[run])
             for k in range(1, hops + 1)}
    return reach, lag, ready


def batches(hops, ready):
    edges = [9, 11, 13, 14, 15, 16, hops + 1]
    edges = [e for e in edges if e <= hops] + [hops + 1]
    result, low = [], 0
    for edge in edges:
        distances = [k for k in sorted(ready) if low <= ready[k] < edge]
        result.append((edge if edge <= hops else None, ([0] if low == 0 else []) + distances))
        low = edge
    return result


def solution(mesh):
    placed = (
        P(("grp", "ep"), None),
        P(),
        P(("grp", "ep"), None),
        P(("grp", "ep"), None),
        P("ep", None, None),
        P("ep", None, None),
        P("ep", None, None),
    )
    return jax.shard_map(
        layer, mesh=mesh, in_specs=placed, out_specs=P(("grp", "ep"), None), check_vma=False
    )
```

```python
from functools import partial

import jax
import jax.numpy as jnp
from jax import lax
from jax.experimental import pallas as pl
from jax.experimental.pallas import tpu as pltpu
from jax.sharding import PartitionSpec as P


INTERPRET = False
LANES = 128
SUB = 32
LIMIT = 24 * 1024 * 1024
RUNS = 4
EDGES = (9, 11, 12, 14, 16)
META = 16
EPSILON = 1e-05
clamp_limit = 7.0
sigmoid_slope = 1.702
f32 = jnp.float32
bf16 = jnp.bfloat16


def shifted(array, step):
    size = lax.axis_size("ep")
    return lax.ppermute(array, "ep", [(i, (i + step) % size) for i in range(size)])


def iota(shape, axis):
    return lax.broadcasted_iota(jnp.int32, shape, axis)


def reaches(ids, pair, parity, experts):
    half = experts // 2
    ahead = ids - pair
    ahead = jnp.where(ahead < 0, ahead + experts, ahead)
    behind = experts - ahead
    up_even = jnp.where(ahead < half, 2 * ahead + 1, 0)
    up_odd = jnp.where((ahead >= 1) & (ahead <= half), 2 * ahead, 0)
    down_even = jnp.where(ahead >= half, 2 * behind, 0)
    down_odd = jnp.where(ahead == 0, 1, jnp.where(ahead > half, 2 * behind + 1, 0))
    even = parity == 0
    return jnp.where(even, up_even, up_odd), jnp.where(even, down_even, down_odd)


def prepare_kernel(where_ref, tokens_ref, gain_ref, ids_ref, weight_ref,
                   *out_refs, experts):
    rows, width = tokens_ref.shape
    pair, parity = where_ref[0], where_ref[1]
    values = tokens_ref[...].astype(f32)
    center = values - jnp.mean(values, axis=-1, keepdims=True)
    spread = jnp.mean(center * center, axis=-1, keepdims=True)
    normed = (center * lax.rsqrt(spread + EPSILON) * gain_ref[...]).astype(bf16)

    weights = weight_ref[...]
    high = weights.astype(bf16).astype(f32)
    middle = (weights - high).astype(bf16).astype(f32)
    low = weights - high - middle
    sub = iota((rows, rows), 0)
    meta = jnp.zeros((rows, rows), f32)
    entries = [ids_ref[0:1, :].astype(f32), ids_ref[1:2, :].astype(f32)]
    for k in range(2):
        entries += [high[k:k + 1, :], middle[k:k + 1, :], low[k:k + 1, :]]
    for number, entry in enumerate(entries):
        meta = jnp.where(sub == number, entry, meta)
    table = meta.T
    meta_bf = meta[0:META, :].astype(bf16)
    first_c, second_c = table[:, 0:1].astype(jnp.int32), table[:, 1:2].astype(jnp.int32)
    first_r, second_r = ids_ref[0:1, :], ids_ref[1:2, :]
    reach_c = [jnp.maximum(a, b) for a, b in zip(
        reaches(first_c, pair, parity, experts), reaches(second_c, pair, parity, experts))]
    reach_r = [jnp.maximum(a, b) for a, b in zip(
        reaches(first_r, pair, parity, experts), reaches(second_r, pair, parity, experts))]
    sub_i, lane_i = iota((rows, rows), 0), iota((rows, rows), 1)
    blocks = width // LANES
    for way in range(2):
        first_ref, second_ref, late_ref = out_refs[3 * way:3 * way + 3]
        t_ref = out_refs[6 + way]
        col, row = reach_c[way], reach_r[way]
        ahead_c = (row > col) | ((row == col) & (lane_i < sub_i))
        ahead_r = (col > row) | ((col == row) & (sub_i < lane_i))
        rank_c = jnp.sum(ahead_c.astype(f32), axis=1, keepdims=True).astype(jnp.int32)
        rank_r = jnp.sum(ahead_r.astype(f32), axis=0, keepdims=True).astype(jnp.int32)
        back = (rank_c == lane_i).astype(f32).astype(bf16)
        order = (rank_r == sub_i).astype(f32).astype(bf16)
        t_ref[...] = back
        ordered = jnp.dot(order, normed, preferred_element_type=f32).astype(bf16)
        first_ref[SUB * blocks:SUB * blocks + META, :] = jnp.dot(
            meta_bf, back, preferred_element_type=f32).astype(bf16)
        for run, (ref, start) in enumerate(((first_ref, 0), (second_ref, 0),
                                            (second_ref, SUB * blocks), (late_ref, 0))):
            put_run(ref, start, ordered[SUB * run:SUB * (run + 1)])


def put_run(ref, start, rows):
    for c in range(rows.shape[1] // LANES):
        ref[start + SUB * c:start + SUB * (c + 1), :] = rows[:, LANES * c:LANES * (c + 1)]


def result_place(run, size):
    return ((0, 0), (1, 0), (1, size), (0, size))[run]


def result_rows(count, size):
    first = size * (2 if count == RUNS else 1)
    return [first] if count == 1 else [first, size * min(count - 1, 2)]


def get_block(refs, places, c):
    parts = [refs[n][start + SUB * c:start + SUB * (c + 1), :] for n, start in places]
    return parts[0] if len(parts) == 1 else jnp.concatenate(parts, axis=0)


def expert_kernel(*refs, specs, count):
    where_ref = refs[0]
    sources = refs[1:1 + count]
    gate_ref, up_ref, down_ref = refs[1 + count:4 + count]
    results = refs[4 + count:-4]
    rows_ref, sum_ref, hot_ref, factor_ref = refs[-4:]
    width = rows_ref.shape[1]
    blocks = width // LANES
    expert, parity = where_ref[0], where_ref[1]

    before = (iota((LANES, LANES), 0) < iota((LANES, LANES), 1)).astype(f32).astype(bf16)
    lane = iota((1, LANES), 1)
    for number, (places, only) in enumerate(specs):
        index, start = places[0]
        start = start + SUB * blocks
        meta = sources[index][start:start + META, :].astype(f32)
        target = expert.astype(f32)
        valid = lane < SUB * len(places)
        if only is not None:
            valid = valid & (lane < jnp.where(parity == only, LANES, 0))
        first = (meta[0:1] == target) & valid
        second = (meta[1:2] == target) & valid
        factor = jnp.where(first, (meta[2:3] + meta[3:4]) + meta[4:5], 0.0)
        factor = factor + jnp.where(second, (meta[5:6] + meta[6:7]) + meta[7:8], 0.0)
        match = jnp.where(first | second, 1.0, 0.0)
        slot = jnp.dot(jnp.broadcast_to(match, (16, LANES)).astype(bf16), before,
                       preferred_element_type=f32)[0:1]
        slot = jnp.where(match > 0.0, slot, -1.0)
        hot = (slot == iota((SUB, LANES), 0).astype(f32)).astype(f32)
        span = pl.ds(SUB * number, SUB)
        factor_ref[span, :] = jnp.broadcast_to(
            jnp.sum(hot * factor, axis=1, keepdims=True), (SUB, LANES))
        hot_ref[span, :] = hot
        hot = hot[:, :SUB * len(places)].astype(bf16)
        for c in range(blocks):
            rows_ref[span, LANES * c:LANES * (c + 1)] = jnp.dot(
                hot, get_block(sources, places, c), preferred_element_type=f32).astype(bf16)

    hidden = gate_ref.shape[1]
    tile = min(256, hidden)

    def add_tile(number, _):
        span = pl.ds(pl.multiple_of(number * tile, tile), tile)
        rows = rows_ref[...]
        gate = jnp.minimum(jnp.dot(rows, gate_ref[:, span], preferred_element_type=f32), clamp_limit)
        up = jnp.clip(jnp.dot(rows, up_ref[:, span], preferred_element_type=f32),
                      -clamp_limit, clamp_limit)
        active = ((up + 1.0) * (gate * jax.nn.sigmoid(gate * sigmoid_slope))).astype(bf16)
        part = jnp.dot(active, down_ref[span, :], preferred_element_type=f32)
        sum_ref[...] = jnp.where(number == 0, 0.0, sum_ref[...]) + part
        return 0

    lax.fori_loop(0, hidden // tile, add_tile, 0)

    cursor = 0
    for number, (places, _) in enumerate(specs):
        span = pl.ds(SUB * number, SUB)
        weighted = (sum_ref[span, :] * factor_ref[span, 0:1]).astype(bf16)
        spread = hot_ref[span, :].T[:SUB * len(places)].astype(bf16)
        dense = jnp.dot(spread, weighted, preferred_element_type=f32).astype(bf16)
        for run in range(len(places)):
            which, start = result_place(run, SUB * blocks)
            put_run(results[cursor + which], start, dense[SUB * run:SUB * (run + 1)])
        cursor += len(result_rows(len(places), SUB * blocks))


def finish_kernel(*refs, specs):
    *in_refs, upt_ref, downt_ref, out_ref = refs
    blocks = out_ref.shape[1] // LANES
    for c in range(blocks):
        total = None
        for back_ref, places in zip((upt_ref, upt_ref, downt_ref), specs):
            part = jnp.dot(back_ref[...], get_block(in_refs, places, c), preferred_element_type=f32)
            total = part if total is None else total + part
        out_ref[:, LANES * c:LANES * (c + 1)] = total.astype(bf16)


VMEM = pl.BlockSpec(memory_space=pltpu.VMEM)
SMEM = pl.BlockSpec(memory_space=pltpu.SMEM)


def hold_kernel(*refs):
    own, partner, held, sems = refs[0:3], refs[3:6], refs[6:9], refs[9]
    hidden = own[0].shape[2]
    parts = [ref.at[:, pl.ds(0, hidden)] for ref in held[:2]] + [held[2].at[pl.ds(0, hidden), :]]
    copies = [pltpu.make_async_copy(own[n].at[0], parts[n], sems.at[n]) for n in range(3)]
    for copy in copies:
        copy.start()
    held[0][:, hidden:] = partner[0][0]
    held[1][:, hidden:] = partner[1][0]
    held[2][hidden:, :] = partner[2][0]
    for copy in copies:
        copy.wait()


def hold_weights(weights, partner):
    _, width, hidden = weights[0].shape
    shapes = [(width, 2 * hidden)] * 2 + [(2 * hidden, width)]
    return pl.pallas_call(
        hold_kernel,
        in_specs=[pl.BlockSpec(memory_space=pltpu.HBM)] * 3 + [VMEM] * 3,
        out_specs=[VMEM] * 3,
        out_shape=[pltpu.VMEM(shape, bf16) for shape in shapes],
        scratch_shapes=[pltpu.SemaphoreType.DMA((3,))],
        compiler_params=pltpu.CompilerParams(vmem_limit_bytes=28 * 1024 * 1024),
        interpret=INTERPRET,
        name="hold",
    )(*weights, *partner)


def gathered(pieces):
    arrays, specs = [], []
    for places in pieces:
        numbers = []
        for array, start in places:
            found = [n for n, a in enumerate(arrays) if a is array]
            if not found:
                arrays.append(array)
            numbers.append((found[0] if found else len(arrays) - 1, start))
        specs.append(tuple(numbers))
    return arrays, tuple(specs)


def apply_experts(where, pieces, parities, weights):
    width, hidden = weights[0].shape
    arrays, places = gathered(pieces)
    size = SUB * width // LANES
    heights = [n for p in places for n in result_rows(len(p), size)]
    rows = SUB * len(places)
    outs = pl.pallas_call(
        partial(expert_kernel, specs=tuple(zip(places, parities)), count=len(arrays)),
        in_specs=[SMEM] + [VMEM] * (len(arrays) + 3),
        out_specs=[VMEM] * len(heights),
        out_shape=[jax.ShapeDtypeStruct((n, LANES), bf16) for n in heights],
        scratch_shapes=[pltpu.VMEM((rows, width), bf16), pltpu.VMEM((rows, width), f32),
                        pltpu.VMEM((rows, LANES), f32), pltpu.VMEM((rows, LANES), f32)],
        compiler_params=pltpu.CompilerParams(vmem_limit_bytes=LIMIT),
        cost_estimate=pl.CostEstimate(
            flops=6 * rows * width * hidden, transcendentals=0,
            bytes_accessed=6 * width * hidden),
        interpret=INTERPRET,
        name="experts",
    )(where, *arrays, *weights)
    results, cursor = [], 0
    for p in places:
        take = len(result_rows(len(p), size))
        results.append(list(outs[cursor:cursor + take]))
        cursor += take
    return results


def layer(tokens, norm_gain, expert_ids, route_weight, gate_weight, up_weight, down_weight):
    devices = lax.axis_size("ep")
    ring = devices // 2
    experts = ring // 2
    rows, width = tokens.shape
    blocks = width // LANES
    capacity = min(rows, 2 * rows * expert_ids.shape[1] // experts)
    hops = ring // 2
    chip = lax.axis_index("ep") // 2
    where = jnp.stack([chip // 2, chip % 2]).astype(jnp.int32)
    reach, lag, ready = plan(hops, capacity, rows)

    swap = [(i, i ^ 1) for i in range(devices)]
    weights = (gate_weight, up_weight, down_weight)
    partner = []
    for w in weights:
        partner.append(lax.ppermute(w, "ep", swap))

    held = hold_weights(weights, partner)

    size = SUB * blocks
    shapes = [jax.ShapeDtypeStruct((n, LANES), bf16) for n in (size + META, 2 * size, size)]
    outs = pl.pallas_call(
        partial(prepare_kernel, experts=experts),
        in_specs=[SMEM, VMEM, VMEM, VMEM, VMEM],
        out_specs=[VMEM] * 8,
        out_shape=shapes * 2 + [jax.ShapeDtypeStruct((rows, rows), bf16)] * 2,
        interpret=INTERPRET,
        name="prepare",
    )(where, tokens, norm_gain.reshape(1, width), expert_ids.T, route_weight.T)
    mine = {1: outs[0:3], -1: outs[3:6]}
    backs = outs[6:]

    first, second, late = mine[1]
    arrived = {(0, 0): [(first, 0), (second, 0), (second, size), (late, 0)]}
    moving = {way: [mine[way][0], mine[way][1]] for way in (1, -1)}
    for turn in range(1, hops + 1):
        for way in (1, -1):
            first, second = moving[way]
            if turn == lag[3] + 1:
                first = jnp.concatenate([first, mine[way][2]], axis=0)
            if turn == reach[2] + 1:
                second = second[:size]
            first = shifted(first, 2 * way)
            if turn <= reach[1]:
                second = shifted(second, 2 * way)
            moving[way] = [first, second]
            starts = [(first, 0), (second, 0), (second, size), (first, size + META)]
            for run in range(RUNS):
                k = turn - lag[run]
                if 1 <= k <= reach[run]:
                    arrived.setdefault((way, k), [None] * RUNS)[run] = starts[run]

    given = {}
    for _, distances in batches(hops, ready):
        keys = [(way, k) if k else (0, 0) for k in distances for way in ((1, -1) if k else (1,))]
        pieces = [[p for p in arrived[key] if p is not None] for key in keys]
        parities = [None if k < hops else (1 if way == 1 else 0) for way, k in keys]
        values = apply_experts(where, pieces, parities, held)
        given.update(zip(keys, values))

    totals = {way: given[way, hops] for way in (1, -1)}
    for k in range(hops - 1, -1, -1):
        for way in (1, -1):
            came = [shifted(x, -2 * way)
                    for x in totals[way]]
            if k == 0:
                totals[way] = came
                continue
            joined = []
            for number, value in enumerate(given[way, k]):
                if number < len(came):
                    more = came[number]
                    padded = jnp.pad(more, ((0, value.shape[0] - more.shape[0]), (0, 0)))
                    value = (value.astype(f32) + padded.astype(f32)).astype(bf16)
                joined.append(value)
            totals[way] = joined

    ends = []
    for pair in (given[0, 0], totals[1], totals[-1]):
        ends.append([(pair[which], start)
                     for which, start in (result_place(run, size) for run in range(RUNS))])
    arrays, places = gathered(ends)
    return pl.pallas_call(
        partial(finish_kernel, specs=places),
        in_specs=[VMEM] * (len(arrays) + 2),
        out_specs=VMEM,
        out_shape=jax.ShapeDtypeStruct((rows, width), bf16),
        interpret=INTERPRET,
        name="finish",
    )(*arrays, *backs)


def plan(hops, capacity, rows):
    reach = []
    for run in range(RUNS):
        reach.append(max(k for k in range(1, hops + 1)
                         if min(rows, capacity * (hops // 2 - (k + 1) // 2 + 1)) > SUB * run))
    lag = [0, 0, 0, hops - reach[3]]
    ready = {k: max(k + lag[run] for run in range(RUNS) if k <= reach[run])
             for k in range(1, hops + 1)}
    return reach, lag, ready


def batches(hops, ready):
    edges = [e for e in EDGES if e <= hops] + [hops + 1]
    result, low = [], 0
    for edge in edges:
        distances = [k for k in sorted(ready) if low <= ready[k] < edge]
        result.append((edge if edge <= hops else None, ([0] if low == 0 else []) + distances))
        low = edge
    return result


def solution(mesh):
    placed = (
        P(("grp", "ep"), None),
        P(),
        P(("grp", "ep"), None),
        P(("grp", "ep"), None),
        P("ep", None, None),
        P("ep", None, None),
        P("ep", None, None),
    )
    return jax.shard_map(
        layer, mesh=mesh, in_specs=placed, out_specs=P(("grp", "ep"), None), check_vma=False
    )
```
